32 devices in a mesh: sp: 8 (over z, x), tp: 4 (over y, core).
Axes of the slice: x: 2, y: 2, z: 4, core: 2. Of those that a mesh axis runs over, the one named last changes fastest.
Arguments:
- rows_in: bfloat16 [1024, 2048], P(('sp', 'tp')), may hold values from -8 to 8
- in_gain: float32 [2048], replicated, may hold values from 0.1 to 1.9
- query_down: bfloat16 [2048, 256], replicated, may hold values from -0.125 to 0.125
- query_gain: float32 [256], replicated, may hold values from 0.1 to 1.9
- kv_down: bfloat16 [2048, 128], replicated, may hold values from -0.125 to 0.125
- kv_gain: float32 [128], replicated, may hold values from 0.1 to 1.9
- rope_down: bfloat16 [2048, 64], replicated, may hold values from -0.125 to 0.125
- query_nope_up: bfloat16 [256, 512], P(None, 'tp'), may hold values from -0.375 to 0.375
- query_rope_up: bfloat16 [256, 256], P(None, 'tp'), may hold values from -0.375 to 0.375
- key_up: bfloat16 [128, 512], P(None, 'tp'), may hold values from -2.9811459 to 2.9811459
- value_up: bfloat16 [128, 512], P(None, 'tp'), may hold values from -0.5 to 0.5
- rec_query: bfloat16 [2048, 256], P(None, 'tp'), may hold values from -0.125 to 0.125
- rec_key: bfloat16 [2048, 256], P(None, 'tp'), may hold values from -0.125 to 0.125
- rec_value: bfloat16 [2048, 512], P(None, 'tp'), may hold values from -0.125 to 0.125
- gate_weight: bfloat16 [2048, 4, 4], P(None, None, 'tp'), may hold values from -0.125 to 0.125
- forget_level: float32 [1024, 2, 4], P('sp', None, 'tp'), may hold values from 0 to 14
- head_gain: float32 [512], P('tp'), may hold values from 0.1 to 1.9
- init_state: float32 [2, 4, 64, 128], P(None, 'tp'), may hold values from -96 to 96
- init_norm: float32 [2, 4, 64], P(None, 'tp'), may hold values from -96 to 96
- out_attn: bfloat16 [512, 2048], P('tp'), may hold values from -0.25 to 0.25
- out_rec: bfloat16 [512, 2048], P('tp'), may hold values from -0.25 to 0.25
Outputs:
- mixed_out: bfloat16 [1024, 2048], P(('sp', 'tp'))
The draws below stay inside these ranges and needn't reach their ends.
All inputs are finite; a program needn't handle non-finite values.
Results may differ from the reference program's by a relative error of at most 0.023.
Values may be sent and summed in bfloat16 or wider, within the bound.
A program may use at most 64 MiB of HBM per device.

```python
import math
import jax
import jax.numpy as jnp
from jax import lax

D = 2048
HA = 4
RECURRENT_HEADS = 4
QL = 256
KVL = 128
NOPE = 128
ROPE = 64
VH = 128
MK = 64
MV = 128
MBLOCK = 128
SEQUENCE_TOKENS = 1024
HAG = 1
HMG = 1
N_TP = 4


def draw_rows_in(key, part):
    key_noise = jax.random.fold_in(key, 11)
    key_means = jax.random.fold_in(key, 12)
    regions = 64
    region_of = jnp.arange(SEQUENCE_TOKENS) * regions // SEQUENCE_TOKENS
    noise = jax.random.normal(key_noise, (SEQUENCE_TOKENS, D), jnp.float32)
    centres = 0.7 * jax.random.normal(key_means, (regions, D), jnp.float32)
    values = jnp.clip(noise + centres[region_of], -8.0, 8.0)
    return values.astype(jnp.bfloat16)


def draw_key_up(key, part):
    key_base = jax.random.fold_in(key, 31)
    base = jnp.clip(jax.random.normal(key_base, (KVL, HA, NOPE), jnp.float32), -4.0, 4.0) * KVL ** (-0.5)
    return base.reshape(KVL, HA * NOPE).astype(jnp.bfloat16)


def draw_forget_level(key, part):
    key_slow = jax.random.fold_in(key, 21)
    key_shift = jax.random.fold_in(key, 22)
    key_spike = jax.random.fold_in(key, 23)
    slow_heads = jax.random.bernoulli(key_slow, 0.5, (2, RECURRENT_HEADS))
    floor_level_value = jnp.where(slow_heads, jnp.log(4.0 * SEQUENCE_TOKENS), jnp.log(80.0)).astype(jnp.float32)
    blocks = 256
    block_lookup = jnp.arange(SEQUENCE_TOKENS) * blocks // SEQUENCE_TOKENS
    offset_steps = jax.random.uniform(key_shift, (blocks, 2, RECURRENT_HEADS), jnp.float32, -0.7, 0.7)
    spike_position = jax.random.randint(key_spike, (2, 2, RECURRENT_HEADS), 0, SEQUENCE_TOKENS)
    spike_match = jnp.any(jnp.arange(SEQUENCE_TOKENS)[:, None, None, None] == spike_position[None], axis=1)
    level_value = jnp.where(spike_match, 0.8, floor_level_value[None] + offset_steps[block_lookup])
    return level_value.astype(jnp.float32)


def block_levels(key, dims, split, low, top_value):
    level = 1.0
    for dim, parts in split:
        draws = jax.random.uniform(jax.random.fold_in(jax.random.fold_in(key, 6), dim), (parts,), jnp.float32, low / len(split), top_value / len(split))
        level = level * jnp.repeat(jnp.exp(draws), dims[dim] // parts).reshape((-1,) + (1,) * (len(dims) - 1 - dim))
    return level


def gaussian(key, extent, spread, most, split=(), kind=jnp.bfloat16):
    level = block_levels(key, extent, split, -0.22, 0.18) if split else 1.0
    drawn = jax.random.normal(key, extent, jnp.float32) * spread * level
    return jnp.minimum(jnp.maximum(drawn, -most), most).astype(kind)


def setup_inputs(seed: int = 0) -> dict:
    splits = jax.random.split(jax.random.key(seed), 22)
    rows_in = draw_rows_in(jax.random.fold_in(splits[21], 71), 0)
    in_gain = jnp.clip(1.0 + 0.18 * jax.random.normal(splits[1], (D,), jnp.float32), 0.1, 1.9)
    query_down = gaussian(splits[2], (D, QL), D ** -0.5, 0.125)
    query_gain = jnp.clip(1.0 + 0.18 * jax.random.normal(splits[3], (QL,), jnp.float32), 0.1, 1.9)
    kv_down = gaussian(splits[4], (D, KVL), D ** -0.5, 0.125)
    kv_gain = jnp.clip(1.0 + 0.18 * jax.random.normal(splits[5], (KVL,), jnp.float32), 0.1, 1.9)
    rope_down = gaussian(splits[6], (D, ROPE), D ** -0.5, 0.125)
    query_nope_up = gaussian(splits[7], (QL, HA * NOPE), QL ** -0.5, 0.375, ((1, 4),))
    query_rope_up = gaussian(splits[8], (QL, HA * ROPE), QL ** -0.5, 0.375, ((1, 4),))
    key_up = draw_key_up(jax.random.fold_in(splits[21], 71), 0)
    value_up = gaussian(splits[10], (KVL, HA * VH), KVL ** -0.5, 0.5, ((1, 4),))
    rec_query = gaussian(splits[11], (D, RECURRENT_HEADS * MK), D ** -0.5, 0.125, ((1, 4),))
    rec_key = gaussian(splits[12], (D, RECURRENT_HEADS * MK), D ** -0.5, 0.125, ((1, 4),))
    rec_value = gaussian(splits[13], (D, RECURRENT_HEADS * MV), D ** -0.5, 0.125, ((1, 4),))
    gate_weight = gaussian(splits[14], (D, 4, RECURRENT_HEADS), D ** -0.5, 0.125, ((2, 4),))
    forget_level = draw_forget_level(jax.random.fold_in(splits[21], 71), 0)
    head_gain = jnp.clip(1.0 + 0.18 * jax.random.normal(splits[16], (RECURRENT_HEADS * MV,), jnp.float32), 0.1, 1.9)
    init_state = gaussian(splits[17], (2, RECURRENT_HEADS, MK, MV), (0.5 * SEQUENCE_TOKENS ** 0.5), 96.0, ((1, 4),), jnp.float32)
    init_norm = gaussian(splits[18], (2, RECURRENT_HEADS, MK), (0.5 * SEQUENCE_TOKENS ** 0.5), 96.0, ((1, 4),), jnp.float32)
    out_attn = gaussian(splits[19], (HA * VH, D), (HA * VH) ** -0.5, 0.25, ((0, 4),))
    out_rec = gaussian(splits[20], (RECURRENT_HEADS * MV, D), (RECURRENT_HEADS * MV) ** -0.5, 0.25, ((0, 4),))
    return dict(rows_in=rows_in, in_gain=in_gain, query_down=query_down, query_gain=query_gain, kv_down=kv_down, kv_gain=kv_gain, rope_down=rope_down, query_nope_up=query_nope_up, query_rope_up=query_rope_up, key_up=key_up, value_up=value_up, rec_query=rec_query, rec_key=rec_key, rec_value=rec_value, gate_weight=gate_weight, forget_level=forget_level, head_gain=head_gain, init_state=init_state, init_norm=init_norm, out_attn=out_attn, out_rec=out_rec)


EPS = 1e-06
NEG = -1e+30

def rms_rows(values, gains):
    return values * lax.rsqrt(lax.optimization_barrier(jnp.mean(values * values, axis=-1, keepdims=True)) + EPS) * gains.astype(jnp.float32)

def rotate(values, positions):
    half_len = values.shape[-1] // 2
    frequency = 10000.0 ** (-jnp.arange(half_len, dtype=jnp.float32) / half_len)
    angles = positions.astype(jnp.float32)[:, None] * frequency[None, :]
    angles = jnp.concatenate([angles, angles], axis=-1)[:, None, :]
    turned = jnp.concatenate([-values[..., half_len:], values[..., :half_len]], axis=-1)
    return values * jnp.cos(angles) + turned * jnp.sin(angles)

def recurrence(query, keys_in, value_in, log_in, log_keep, c_start, n_start, m_start, floor_value):
    head_count, seq_len = log_in.shape
    block_count = seq_len // MBLOCK
    lower_mask = jnp.tril(jnp.ones((MBLOCK, MBLOCK), bool))
    highest = lax.Precision.HIGHEST

    def to_blocks(array):
        return jnp.moveaxis(array.reshape((head_count, block_count, MBLOCK) + array.shape[2:]), 1, 0)

    def one_step(carried, inputs):
        c_state, n_state, m_state = carried
        q_block, k_block, v_block, in_block, keep_block = inputs
        log_cum = jnp.cumsum(keep_block, axis=-1)
        log_decay = jnp.where(lower_mask, log_cum[:, :, None] - log_cum[:, None, :] + in_block[:, None, :], NEG)
        carry_log = log_cum + m_state[:, None]
        row_max = jnp.maximum(lax.optimization_barrier(jnp.max(log_decay, axis=-1)), carry_log)
        gated = jnp.einsum('htd,hsd->hts', q_block, k_block, precision=highest) * jnp.exp(log_decay - row_max[..., None])
        carry_weight = jnp.exp(carry_log - row_max)
        numerator = jnp.einsum('hts,hse->hte', gated, v_block, precision=highest) + carry_weight[..., None] * jnp.einsum('htd,hde->hte', q_block, c_state, precision=highest)
        denominator = lax.optimization_barrier(jnp.sum(gated, axis=-1)) + carry_weight * jnp.einsum('htd,hd->ht', q_block, n_state, precision=highest)
        result = numerator / jnp.maximum(jnp.abs(denominator), floor_value * jnp.exp(-row_max))[..., None]
        cum_end = log_cum[:, -1]
        weight_log = cum_end[:, None] - log_cum + in_block
        new_max = jnp.maximum(cum_end + m_state, lax.optimization_barrier(jnp.max(weight_log, axis=-1)))
        decay_all = jnp.exp(cum_end + m_state - new_max)
        in_weights = jnp.exp(weight_log - new_max[:, None])
        c_state = decay_all[:, None, None] * c_state + jnp.einsum('hsd,hse->hde', k_block * in_weights[..., None], v_block, precision=highest)
        n_state = decay_all[:, None] * n_state + jnp.einsum('hs,hsd->hd', in_weights, k_block, precision=highest)
        return ((c_state, n_state, new_max), result)
    inputs = tuple((to_blocks(array) for array in (query, keys_in, value_in, log_in, log_keep)))
    _, outputs = lax.scan(one_step, (c_start, n_start, m_start), inputs)
    return jnp.moveaxis(outputs, 0, 1).reshape(head_count, seq_len, -1)

def heads_first(product, head_width):
    rounded = lax.optimization_barrier(product.astype(jnp.bfloat16))
    return rounded.astype(jnp.float32).reshape(product.shape[0], -1, head_width).transpose(1, 0, 2)

def reference(rows_in, in_gain, query_down, query_gain, kv_down, kv_gain, rope_down, query_nope_up, query_rope_up, key_up, value_up, rec_query, rec_key, rec_value, gate_weight, forget_level, head_gain, init_state, init_norm, out_attn, out_rec):
    f32 = jnp.float32
    bf16 = jnp.bfloat16
    positions = jnp.arange(SEQUENCE_TOKENS, dtype=jnp.int32)
    normed = rms_rows(rows_in.astype(f32), in_gain).astype(bf16)
    q_latent = rms_rows(jnp.dot(normed, query_down, preferred_element_type=f32), query_gain).astype(bf16)
    kv_latent = rms_rows(jnp.dot(normed, kv_down, preferred_element_type=f32), kv_gain).astype(bf16)
    key_rope = rotate(jnp.dot(normed, rope_down, preferred_element_type=f32)[:, None, :], positions)[:, 0, :].astype(bf16)
    query_nope = jnp.dot(q_latent, query_nope_up, preferred_element_type=f32).astype(bf16).reshape(SEQUENCE_TOKENS, HA, NOPE)
    query_rope = rotate(jnp.dot(q_latent, query_rope_up, preferred_element_type=f32).reshape(SEQUENCE_TOKENS, HA, ROPE), positions).astype(bf16)
    query_abs = jnp.einsum('thn,khn->thk', query_nope.astype(f32), key_up.astype(f32).reshape(KVL, HA, NOPE)).astype(bf16)
    queries = jnp.concatenate([query_abs, query_rope], axis=-1)
    key_rows = jnp.concatenate([kv_latent, key_rope], axis=-1)
    score_scale = (NOPE + ROPE) ** (-0.5)
    query_block = math.gcd(SEQUENCE_TOKENS, 128)

    def attend_block(block_q):
        rows_q = block_q.reshape(query_block * HA, KVL + ROPE)
        scores = jnp.dot(rows_q, key_rows.T, preferred_element_type=f32) * score_scale
        row_top = lax.optimization_barrier(jnp.max(scores, axis=-1, keepdims=True))
        expo_all = jnp.exp(scores - row_top)
        totals = lax.optimization_barrier(jnp.sum(expo_all, axis=-1, keepdims=True))
        latent = (jnp.dot(expo_all.astype(bf16), kv_latent, preferred_element_type=f32) / totals).astype(bf16)
        return latent.reshape(query_block, HA, KVL)
    attended = lax.map(attend_block, queries.reshape(SEQUENCE_TOKENS // query_block, query_block, HA, KVL + ROPE)).reshape(SEQUENCE_TOKENS, HA, KVL)
    attention_out = jnp.einsum('thk,khv->thv', attended.astype(f32), value_up.astype(f32).reshape(KVL, HA, VH)).astype(bf16).reshape(SEQUENCE_TOKENS, HA * VH)
    rec_q = heads_first(jnp.dot(normed, rec_query, preferred_element_type=f32), MK)
    rec_k = heads_first(jnp.dot(normed, rec_key, preferred_element_type=f32), MK) * MK ** (-0.5)
    rec_v = heads_first(jnp.dot(normed, rec_value, preferred_element_type=f32), MV)
    gate_pre = jnp.einsum('td,dgh->tgh', normed.astype(f32), gate_weight.astype(f32))
    input_fwd = gate_pre[:, 0].T
    keep_fwd = jax.nn.log_sigmoid(gate_pre[:, 1] + forget_level[:, 0]).T
    input_bwd = gate_pre[:, 2].T
    keep_bwd = jax.nn.log_sigmoid(gate_pre[:, 3] + forget_level[:, 1]).T
    zero_heads = jnp.zeros((RECURRENT_HEADS,), f32)
    floor_value = float(SEQUENCE_TOKENS) ** 0.5
    forward_h = recurrence(rec_q, rec_k, rec_v, input_fwd, keep_fwd, init_state[0], init_norm[0], zero_heads, floor_value)
    backward_h = recurrence(rec_q[:, ::-1], rec_k[:, ::-1], rec_v[:, ::-1], input_bwd[:, ::-1], keep_bwd[:, ::-1], init_state[1], init_norm[1], zero_heads, floor_value)[:, ::-1]
    summed = (forward_h + backward_h).transpose(1, 0, 2)
    recurrent_out = rms_rows(summed, head_gain.reshape(RECURRENT_HEADS, MV)).astype(bf16).reshape(SEQUENCE_TOKENS, RECURRENT_HEADS * MV)
    mixed_out = jnp.zeros((SEQUENCE_TOKENS, D), f32)
    for group in range(N_TP):
        att_cols = attention_out[:, group * HAG * VH:(group + 1) * HAG * VH]
        rec_cols = recurrent_out[:, group * HMG * MV:(group + 1) * HMG * MV]
        partial_value = jnp.dot(att_cols, out_attn[group * HAG * VH:(group + 1) * HAG * VH], preferred_element_type=f32)
        partial_value = partial_value + jnp.dot(rec_cols, out_rec[group * HMG * MV:(group + 1) * HMG * MV], preferred_element_type=f32)
        mixed_out = mixed_out + partial_value.astype(bf16).astype(f32)
    return mixed_out.astype(bf16)
```

```python
import functools

import jax
import jax.numpy as jnp
import numpy as np
from jax import lax
from jax.experimental import pallas as pl
from jax.experimental.pallas import tpu as pltpu
from jax.sharding import PartitionSpec as P

EPS = 1e-06
NEG = -1e30
HIGHEST = lax.Precision.HIGHEST
MESH = pl.DeviceIdType.MESH
F32 = jnp.float32
BF16 = jnp.bfloat16


def dot(a, b, **kw):
    return jnp.dot(a, b, preferred_element_type=F32, **kw)


def dot_t(a, b, **kw):
    return lax.dot_general(a, b, (((1,), (1,)), ((), ())), preferred_element_type=F32, **kw)


def dot_tn(a, b, **kw):
    return lax.dot_general(a, b, (((0,), (0,)), ((), ())), preferred_element_type=F32, **kw)


def rms(values, gains):
    return values * lax.rsqrt(jnp.mean(values * values, axis=-1, keepdims=True) + EPS) * gains


def turned(values):
    half = values.shape[-1] // 2
    return jnp.concatenate([-values[:, half:], values[:, :half]], axis=1)


def three_terms(value):
    high = value.astype(BF16).astype(F32)
    mid = (value - high).astype(BF16).astype(F32)
    return high, mid, value - high - mid


def kernel(n_sp, n_tp, names, *refs):
    count = len(names)
    hbm = dict(zip(names, refs[:count]))
    out_ref = refs[count]
    vm = dict(zip(names, refs[count + 1 : 2 * count + 1]))
    (
        xall,
        kvbuf,
        qcat,
        mix,
        smsg,
        sbuf,
        psend,
        pfull,
        prem,
        plast,
        plast_in,
        load_sem,
        x_send,
        x_recv,
        kv_send,
        kv_fwd,
        kv_recv,
        s_send,
        s_recv,
        p_send,
        p_recv,
        l_send,
        l_recv,
    ) = refs[2 * count + 1 :]
    half = n_tp // 2
    sp = lax.axis_index("sp")
    tp = lax.axis_index("tp")
    parity = lax.rem(tp, 2)
    partner_t = tp + 1 - 2 * parity
    partner = (sp, partner_t)
    rows = xall.shape[1]
    block = n_tp * rows
    plane = n_sp * half
    mine = sp * half + tp // 2

    loads = {
        name: pltpu.make_async_copy(hbm[name], vm[name], load_sem.at[i])
        for i, name in enumerate(names)
    }
    for name in names:
        loads[name].start()

    def peer_of(i):
        linear = lax.rem(mine + i, plane)
        return (linear // half, 2 * lax.rem(linear, half) + parity)

    barrier = pltpu.get_barrier_semaphore()

    def greet(i, c):
        pl.semaphore_signal(barrier, inc=1, device_id=peer_of(i), device_id_type=MESH)
        return c

    lax.fori_loop(1, plane, greet, 0)
    pl.semaphore_signal(barrier, inc=1, device_id=partner, device_id_type=MESH)

    def get(name):
        loads[name].wait()
        return vm[name]

    rows_in = get("rows_in")
    in_gain = get("in_gain")
    xall[tp] = rms(rows_in[...].astype(F32), in_gain[...]).astype(BF16)
    pl.semaphore_wait(barrier, plane)

    def remote(src, dst, send, recv, device):
        return pltpu.make_async_remote_copy(
            src_ref=src,
            dst_ref=dst,
            send_sem=send,
            recv_sem=recv,
            device_id=device,
            device_id_type=MESH,
        )

    def x_copy(slot, k, device):
        return remote(xall.at[slot], xall.at[slot], x_send.at[k], x_recv.at[slot], device)

    def tp_same(d):
        return lax.rem(tp + 2 * d, n_tp)

    x_out = []
    for d in range(1, half):
        x_out.append(x_copy(tp, d, (sp, tp_same(d))))
    x_out.append(x_copy(tp, 0, partner))
    for copy in x_out:
        copy.start()

    own = xall[tp]
    cos_l = get("cos_local")
    sin_l = get("sin_local")
    cos_b = get("cos_base")[sp]
    sin_b = get("sin_base")[sp]
    own_at = pl.ds(pl.multiple_of(tp * rows, rows), rows)
    kv = rms(dot(own, get("kv_down")[...]), get("kv_gain")[...])
    kr = dot(own, get("rope_down")[...])
    c_l = cos_l[own_at, :]
    s_l = sin_l[own_at, :]
    kr = kr * (cos_b * c_l - sin_b * s_l) + turned(kr) * (sin_b * c_l + cos_b * s_l)
    lat = kv.shape[1]
    rope = kr.shape[1]
    slot_me = sp * n_tp + tp
    kvbuf[slot_me, :, :lat] = kv.astype(BF16)
    kvbuf[slot_me, :, lat:] = jnp.concatenate([kr, jnp.zeros_like(kr)], axis=1).astype(BF16)

    def kv_copy(i):
        return remote(
            kvbuf.at[slot_me], kvbuf.at[slot_me], kv_send.at[i], kv_recv.at[slot_me], peer_of(i)
        )

    def slot_of(i):
        s, t = peer_of(i)
        return s * n_tp + t

    def kv_relay(i):
        slot = slot_of(i)
        return remote(kvbuf.at[slot], kvbuf.at[slot], kv_fwd.at[i], kv_recv.at[slot], partner)

    def start_kv(i, c):
        kv_copy(i).start()
        return c

    lax.fori_loop(1, plane, start_kv, 0)
    kv_relay(0).start()

    x_fwd = []
    for d in range(1, half):
        slot = tp_same(d)
        x_copy(slot, 0, partner).wait_recv()
        copy = x_copy(slot, half + d, partner)
        copy.start()
        x_fwd.append(copy)
    for d in range(half):
        x_copy(lax.rem(partner_t + 2 * d, n_tp), 0, partner).wait_recv()
    x = xall[...].reshape(block, xall.shape[2])

    gates = dot_t(get("gate_rows")[...], x)[:8]
    level = gates + get("levels")[...]
    keep = jnp.minimum(level, 0.0) - jnp.log1p(jnp.exp(-jnp.abs(level)))
    r_id = lax.broadcasted_iota(jnp.int32, (block, block), 0)
    c_id = lax.broadcasted_iota(jnp.int32, (block, block), 1)
    lower = r_id >= c_id
    upper = r_id <= c_id
    cum_f = dot(keep, upper.astype(F32), precision=HIGHEST)[1:2]
    cum_b = dot(keep, lower.astype(F32), precision=HIGHEST)[3:4]
    a_f = gates[0:1] - cum_f
    a_b = gates[2:3] - cum_b
    end_f = cum_f[:, block - 1 : block]
    end_b = cum_b[:, 0:1]
    peak_f = jnp.max(end_f + a_f, axis=1, keepdims=True)
    peak_b = jnp.max(end_b + a_b, axis=1, keepdims=True)
    e_f = jnp.exp(end_f + a_f - peak_f)
    e_b = jnp.exp(end_b + a_b - peak_b)
    row8 = lax.broadcasted_iota(jnp.int32, (8, block), 0)
    stack = jnp.where(
        row8 == 0,
        cum_f,
        jnp.where(row8 == 1, cum_b, jnp.where(row8 == 2, e_f, e_b)),
    )
    eye = (r_id == c_id).astype(F32)
    columns = dot_t(eye, stack, precision=HIGHEST)
    cum_f_col = columns[:, 0:1]
    cum_b_col = columns[:, 1:2]
    e_f_col = columns[:, 2:3]
    e_b_col = columns[:, 3:4]

    k = dot(x, get("rec_key")[...]).astype(BF16).astype(F32)
    k = k * k.shape[1] ** (-0.5)
    v = dot(x, get("rec_value")[...]).astype(BF16)
    k16 = k.astype(BF16)
    mk = k.shape[1]
    mv = v.shape[1]
    n_both = dot(stack.astype(BF16), k16)
    row16 = lax.broadcasted_iota(jnp.int32, (16, mv), 0)

    def put_state(d, e_col, n_row, peak, end):
        smsg[d, :mk, :] = dot_tn((k * e_col).astype(BF16), v).astype(BF16)
        p1, p2, p3 = three_terms(peak)
        f1, f2, f3 = three_terms(end)
        tail = jnp.concatenate([n_row, jnp.zeros((1, mv - mk), F32)], axis=1)
        tail = jnp.where(row16 == 0, tail, 0.0)
        for at, term in enumerate((p1, p2, p3, f1, f2, f3)):
            tail = jnp.where(row16 == at + 1, term, tail)
        smsg[d, mk:, :] = tail.astype(BF16)

    put_state(0, e_f_col, n_both[2:3], peak_f, end_f)
    put_state(1, e_b_col, n_both[3:4], peak_b, end_b)

    def s_copy(i):
        to = lax.rem(sp + i, n_sp)
        which = jnp.where(to > sp, 0, 1)
        return remote(smsg.at[which], sbuf.at[sp], s_send.at[i], s_recv.at[sp], (to, tp))

    def start_s(i, c):
        s_copy(i).start()
        return c

    lax.fori_loop(1, n_sp, start_s, 0)

    q_latent = rms(dot(x, get("query_down")[...]), get("query_gain")[...]).astype(BF16)
    q_nope = dot(q_latent, get("query_nope_up")[...]).astype(BF16)
    q_rope = dot(q_latent, get("query_rope_up")[...])
    cos_q = cos_b * cos_l[...] - sin_b * sin_l[...]
    sin_q = sin_b * cos_l[...] + cos_b * sin_l[...]
    q_rope = q_rope * cos_q + turned(q_rope) * sin_q
    qcat[:, :lat] = dot_t(q_nope, get("key_up")[...]).astype(BF16)
    qcat[:, lat:] = jnp.concatenate([q_rope, jnp.zeros_like(q_rope)], axis=1).astype(BF16)
    scale = (q_nope.shape[1] + rope) ** (-0.5)

    def relay(i, c):
        slot = slot_of(i)
        remote(
            kvbuf.at[slot], kvbuf.at[slot], kv_send.at[i], kv_recv.at[slot], partner
        ).wait_recv()
        kv_relay(i).start()
        return c

    lax.fori_loop(1, plane, relay, 0)

    q16 = dot(x, get("rec_query")[...]).astype(BF16)
    qf = q16.astype(F32)
    qk = dot_t(q16, k16)

    def within(mask, cum_col, a_row):
        decay = jnp.where(mask, cum_col + a_row, NEG)
        top = jnp.max(decay, axis=1, keepdims=True)
        gated = qk * jnp.exp(decay - top)
        return top, dot(gated.astype(BF16), v), jnp.sum(gated, axis=1, keepdims=True)

    in_f = within(lower, cum_f_col, a_f)
    in_b = within(upper, cum_b_col, a_b)

    def wait_kv(i, c):
        s = i // half
        t = 2 * lax.rem(i, half) + 1 - parity
        slot = s * n_tp + t
        remote(
            kvbuf.at[slot], kvbuf.at[slot], kv_fwd.at[0], kv_recv.at[slot], partner
        ).wait_recv()
        return c

    lax.fori_loop(0, plane, wait_kv, 0)
    queries = qcat[...]
    slots = n_sp * n_tp
    step = min(slots, 32)

    def attend(j, running):
        peak, mass, accum = running
        keys = kvbuf[pl.ds(j * step, step)].reshape(step * rows, kvbuf.shape[2])
        scores = dot_t(queries, keys) * scale
        new = jnp.maximum(peak, jnp.max(scores, axis=1, keepdims=True))
        expo = jnp.exp(scores - new)
        shrink = jnp.exp(peak - new)
        mass = mass * shrink + jnp.sum(expo, axis=1, keepdims=True)
        accum = accum * shrink + dot(expo.astype(BF16), keys[:, :lat])
        return new, mass, accum

    running = (
        jnp.full((block, 1), NEG, F32),
        jnp.zeros((block, 1), F32),
        jnp.zeros((block, lat), F32),
    )
    if slots == step:
        running = attend(0, running)
    else:
        running = lax.fori_loop(0, slots // step, attend, running)
    attended = (running[2] / running[1]).astype(BF16)
    vh = hbm["value_up"].shape[1]
    mix[:, :vh] = dot(attended, get("value_up")[...]).astype(BF16)

    def absorb(j, state):
        c_state, n_state, m_state = state
        remote(smsg.at[0], sbuf.at[j], s_send.at[0], s_recv.at[j], partner).wait_recv()
        c_new = sbuf[j, :mk, :].astype(F32)
        tail = sbuf[j, mk:, :].astype(F32)
        peak = tail[1:2, 0:1] + tail[2:3, 0:1] + tail[3:4, 0:1]
        end = tail[4:5, 0:1] + tail[5:6, 0:1] + tail[6:7, 0:1]
        top = jnp.maximum(end + m_state, peak)
        carried = jnp.exp(end + m_state - top)
        fresh = jnp.exp(peak - top)
        return (
            carried * c_state + fresh * c_new,
            carried * n_state + fresh * tail[0:1, :mk],
            top,
        )

    state0 = get("init_state")
    norm0 = get("init_norm")
    zero = jnp.zeros((1, 1), F32)
    fwd = lax.fori_loop(0, sp, absorb, (state0[0], norm0[0:1], zero))
    bwd = lax.fori_loop(
        0,
        n_sp - 1 - sp,
        lambda j, state: absorb(n_sp - 1 - j, state),
        (state0[1], norm0[1:2], zero),
    )
    floor = float(n_sp * block) ** 0.5

    def finish(inside, cum_col, state):
        top, num, den = inside
        c_state, n_state, m_state = state
        carry = cum_col + m_state
        new = jnp.maximum(top, carry)
        a = jnp.exp(top - new)
        b = jnp.exp(carry - new)
        num = a * num + b * dot(q16, c_state.astype(BF16))
        den = a * den + b * jnp.sum(qf * n_state, axis=1, keepdims=True)
        return num / jnp.maximum(jnp.abs(den), floor * jnp.exp(-new))

    total = finish(in_f, cum_f_col, fwd) + finish(in_b, cum_b_col, bwd)
    mix[:, vh:] = rms(total, get("head_gain")[...]).astype(BF16)

    w_attn = get("out_attn")
    w_rec = get("out_rec")
    pfull[...] = (dot(mix[:, :vh], w_attn[...]) + dot(mix[:, vh:], w_rec[...])).reshape(pfull.shape)
    p_out = []
    for d in range(half):
        to = lax.rem(partner_t + 2 * (d + 1), n_tp)
        psend[d] = pfull[to].astype(BF16)
        copy = remote(psend.at[d], prem.at[d], p_send.at[d], p_recv.at[d], partner)
        copy.start()
        p_out.append(copy)
    l_out = []
    for d in range(half):
        p_out[d].wait_recv()
        to = tp_same(d + 1)
        both = pfull[to] + prem[d].astype(F32)
        if d < half - 1:
            plast[d] = both.astype(BF16)
            copy = remote(plast.at[d], plast_in.at[d], l_send.at[d], l_recv.at[d], (sp, to))
            copy.start()
            l_out.append(copy)
    for copy in l_out:
        copy.wait_recv()
    for d in range(half - 1):
        both = both + plast_in[d].astype(F32)
    out_ref[...] = both.astype(BF16)

    for copy in x_out + x_fwd + p_out + l_out:
        copy.wait_send()

    def drain_kv(i, c):
        kv_copy(i).wait_send()
        return c

    def drain_relay(i, c):
        kv_relay(i).wait_send()
        return c

    def drain_s(i, c):
        s_copy(i).wait_send()
        return c

    lax.fori_loop(1, plane, drain_kv, 0)
    lax.fori_loop(0, plane, drain_relay, 0)
    lax.fori_loop(1, n_sp, drain_s, 0)


ORDER = (
    "rows_in",
    "in_gain",
    "kv_down",
    "kv_gain",
    "rope_down",
    "cos_local",
    "sin_local",
    "cos_base",
    "sin_base",
    "gate_rows",
    "levels",
    "rec_key",
    "rec_value",
    "query_down",
    "query_gain",
    "query_nope_up",
    "query_rope_up",
    "key_up",
    "rec_query",
    "value_up",
    "init_state",
    "init_norm",
    "head_gain",
    "out_attn",
    "out_rec",
)


def shards(
    n_sp,
    n_tp,
    rows_in,
    in_gain,
    query_down,
    query_gain,
    kv_down,
    kv_gain,
    rope_down,
    query_nope_up,
    query_rope_up,
    key_up,
    value_up,
    rec_query,
    rec_key,
    rec_value,
    gate_weight,
    forget_level,
    head_gain,
    init_state,
    init_norm,
    out_attn,
    out_rec,
):
    rows, width = rows_in.shape
    block = forget_level.shape[0]
    lat = kv_down.shape[1]
    rope = rope_down.shape[1]
    mk = rec_key.shape[1]
    mv = rec_value.shape[1]
    half = n_tp // 2
    pair = rope // 2
    frequency = 10000.0 ** (-np.arange(pair) / pair)
    frequency = np.concatenate([frequency, frequency])
    local = np.arange(block)[:, None] * frequency
    base = (np.arange(n_sp) * block)[:, None, None] * frequency
    gate_rows = jnp.pad(gate_weight[:, :, 0].T, ((0, 12), (0, 0)))
    levels = forget_level[:, :, 0].T
    levels = jnp.pad(levels[:, None, :], ((0, 0), (1, 0), (0, 0))).reshape(4, block)
    levels = jnp.pad(levels, ((0, 4), (0, 0)))
    arrays = dict(
        rows_in=rows_in,
        in_gain=in_gain[None],
        kv_down=kv_down,
        kv_gain=kv_gain[None],
        rope_down=rope_down,
        cos_local=jnp.asarray(np.cos(local), F32),
        sin_local=jnp.asarray(np.sin(local), F32),
        cos_base=jnp.asarray(np.cos(base), F32),
        sin_base=jnp.asarray(np.sin(base), F32),
        gate_rows=gate_rows,
        levels=levels,
        rec_key=rec_key,
        rec_value=rec_value,
        query_down=query_down,
        query_gain=query_gain[None],
        query_nope_up=query_nope_up,
        query_rope_up=query_rope_up,
        key_up=key_up,
        rec_query=rec_query,
        value_up=value_up,
        init_state=init_state[:, 0],
        init_norm=init_norm[:, 0],
        head_gain=head_gain[None],
        out_attn=out_attn,
        out_rec=out_rec,
    )
    operands = [arrays[name] for name in ORDER]
    plane = n_sp * half
    slots = n_sp * n_tp
    dma = pltpu.SemaphoreType.DMA
    scratch = [pltpu.VMEM(a.shape, a.dtype) for a in operands]
    scratch += [
        pltpu.VMEM((n_tp, rows, width), BF16),
        pltpu.VMEM((slots, rows, lat + 2 * rope), BF16),
        pltpu.VMEM((block, lat + 2 * rope), BF16),
        pltpu.VMEM((block, value_up.shape[1] + mv), BF16),
        pltpu.VMEM((2, mk + 16, mv), BF16),
        pltpu.VMEM((n_sp, mk + 16, mv), BF16),
        pltpu.VMEM((half, rows, width), BF16),
        pltpu.VMEM((n_tp, rows, width), F32),
        pltpu.VMEM((half, rows, width), BF16),
        pltpu.VMEM((half, rows, width), BF16),
        pltpu.VMEM((half, rows, width), BF16),
        dma((len(operands),)),
        dma((n_tp,)),
        dma((n_tp,)),
        dma((plane,)),
        dma((plane,)),
        dma((slots,)),
        dma((n_sp,)),
        dma((n_sp,)),
        dma((half,)),
        dma((half,)),
        dma((half,)),
        dma((half,)),
    ]
    return pl.pallas_call(
        functools.partial(kernel, n_sp, n_tp, ORDER),
        out_shape=jax.ShapeDtypeStruct((rows, width), BF16),
        in_specs=[pl.BlockSpec(memory_space=pl.ANY)] * len(operands),
        out_specs=pl.BlockSpec(memory_space=pltpu.VMEM),
        scratch_shapes=scratch,
        compiler_params=pltpu.CompilerParams(
            collective_id=0, has_side_effects=True, vmem_limit_bytes=60 * 2**20
        ),
    )(*operands)


def solution(mesh):
    in_specs = (
        P(("sp", "tp"), None),
        P(),
        P(),
        P(),
        P(),
        P(),
        P(),
        P(None, "tp"),
        P(None, "tp"),
        P(None, "tp"),
        P(None, "tp"),
        P(None, "tp"),
        P(None, "tp"),
        P(None, "tp"),
        P(None, None, "tp"),
        P("sp", None, "tp"),
        P("tp"),
        P(None, "tp", None, None),
        P(None, "tp", None),
        P("tp", None),
        P("tp", None),
    )
    return jax.shard_map(
        functools.partial(shards, mesh.shape["sp"], mesh.shape["tp"]),
        mesh=mesh,
        in_specs=in_specs,
        out_specs=P(("sp", "tp"), None),
        check_vma=False,
    )
```

```python
import functools

import jax
import jax.numpy as jnp
import numpy as np
from jax import lax
from jax.experimental import pallas as pl
from jax.experimental.pallas import tpu as pltpu
from jax.sharding import PartitionSpec as P

EPS = 1e-06
NEG = -1e30
HIGHEST = lax.Precision.HIGHEST
MESH = pl.DeviceIdType.MESH
F32 = jnp.float32
BF16 = jnp.bfloat16
STRIPS = 4


def dot(a, b, **kw):
    return jnp.dot(a, b, preferred_element_type=F32, **kw)


def dot_t(a, b, **kw):
    return lax.dot_general(a, b, (((1,), (1,)), ((), ())), preferred_element_type=F32, **kw)


def dot_tn(a, b, **kw):
    return lax.dot_general(a, b, (((0,), (0,)), ((), ())), preferred_element_type=F32, **kw)


def rms(values, gains):
    return values * lax.rsqrt(jnp.mean(values * values, axis=-1, keepdims=True) + EPS) * gains


def turned(values):
    half = values.shape[-1] // 2
    return jnp.concatenate([-values[:, half:], values[:, :half]], axis=1)


def three_terms(value):
    high = value.astype(BF16).astype(F32)
    mid = (value - high).astype(BF16).astype(F32)
    return high, mid, value - high - mid


def kernel(n_sp, n_tp, names, *refs):
    count = len(names)
    hbm = dict(zip(names, refs[:count]))
    out_ref = refs[count]
    vm = dict(zip(names, refs[count + 1 : 2 * count + 1]))
    (
        xall,
        kvbuf,
        qcat,
        mix,
        smsg,
        sbuf,
        psend,
        pfull,
        prem,
        plast,
        plast_in,
        load_sem,
        x_send,
        x_recv,
        kv_send,
        kv_fwd,
        kv_recv,
        s_send,
        s_recv,
        p_send,
        p_recv,
        l_send,
        l_recv,
    ) = refs[2 * count + 1 :]
    half = n_tp // 2
    sp = lax.axis_index("sp")
    tp = lax.axis_index("tp")
    parity = lax.rem(tp, 2)
    partner_t = tp + 1 - 2 * parity
    partner = (sp, partner_t)
    rows = xall.shape[1]
    block = n_tp * rows
    plane = n_sp * half
    mine = sp * half + tp // 2

    loads = {
        name: pltpu.make_async_copy(hbm[name], vm[name], load_sem.at[i])
        for i, name in enumerate(names)
    }
    for name in names:
        loads[name].start()

    def peer_of(i):
        linear = lax.rem(mine + i, plane)
        return (linear // half, 2 * lax.rem(linear, half) + parity)

    barrier = pltpu.get_barrier_semaphore()

    def greet(i, c):
        pl.semaphore_signal(barrier, inc=1, device_id=peer_of(i), device_id_type=MESH)
        return c

    lax.fori_loop(1, plane, greet, 0)
    pl.semaphore_signal(barrier, inc=1, device_id=partner, device_id_type=MESH)

    def get(name):
        loads[name].wait()
        return vm[name]

    rows_in = get("rows_in")
    in_gain = get("in_gain")
    xall[tp] = rms(rows_in[...].astype(F32), in_gain[...]).astype(BF16)
    pl.semaphore_wait(barrier, plane)

    def remote(src, dst, send, recv, device):
        return pltpu.make_async_remote_copy(
            src_ref=src,
            dst_ref=dst,
            send_sem=send,
            recv_sem=recv,
            device_id=device,
            device_id_type=MESH,
        )

    def x_copy(slot, k, device):
        return remote(xall.at[slot], xall.at[slot], x_send.at[k], x_recv.at[slot], device)

    def tp_same(d):
        return lax.rem(tp + 2 * d, n_tp)

    x_out = []
    for d in range(1, half):
        x_out.append(x_copy(tp, d, (sp, tp_same(d))))
    x_out.append(x_copy(tp, 0, partner))
    for copy in x_out:
        copy.start()

    own = xall[tp]
    cos_l = get("cos_local")
    sin_l = get("sin_local")
    cos_b = get("cos_base")[sp]
    sin_b = get("sin_base")[sp]
    own_at = pl.ds(pl.multiple_of(tp * rows, rows), rows)
    kv = rms(dot(own, get("kv_down")[...]), get("kv_gain")[...])
    kr = dot_t(own, get("rope_rows")[...])
    c_l = cos_l[own_at, :]
    s_l = sin_l[own_at, :]
    kr = kr * (cos_b * c_l - sin_b * s_l) + turned(kr) * (sin_b * c_l + cos_b * s_l)
    lat = kv.shape[1]
    rope = kr.shape[1]
    slot_me = sp * n_tp + tp
    kvbuf[slot_me, :, :lat] = kv.astype(BF16)
    kvbuf[slot_me, :, lat:] = jnp.concatenate([kr, jnp.zeros_like(kr)], axis=1).astype(BF16)

    def kv_copy(i):
        return remote(
            kvbuf.at[slot_me], kvbuf.at[slot_me], kv_send.at[i], kv_recv.at[slot_me], peer_of(i)
        )

    def slot_of(i):
        s, t = peer_of(i)
        return s * n_tp + t

    def kv_relay(i):
        slot = slot_of(i)
        return remote(kvbuf.at[slot], kvbuf.at[slot], kv_fwd.at[i], kv_recv.at[slot], partner)

    def start_kv(i, c):
        kv_copy(i).start()
        return c

    lax.fori_loop(1, plane, start_kv, 0)
    kv_relay(0).start()

    x_fwd = []
    for d in range(1, half):
        slot = tp_same(d)
        x_copy(slot, 0, partner).wait_recv()
        copy = x_copy(slot, half + d, partner)
        copy.start()
        x_fwd.append(copy)
    for d in range(half):
        x_copy(lax.rem(partner_t + 2 * d, n_tp), 0, partner).wait_recv()
    x = xall[...].reshape(block, xall.shape[2])

    gates = dot_t(get("gate_rows")[...], x)
    levels = get("levels")
    row4 = lax.broadcasted_iota(jnp.int32, gates.shape, 0)
    level = gates + jnp.where(row4 < 2, levels[0], levels[1])
    keep = jnp.minimum(level, 0.0) - jnp.log1p(jnp.exp(-jnp.abs(level)))
    r_id = lax.broadcasted_iota(jnp.int32, (block, block), 0)
    c_id = lax.broadcasted_iota(jnp.int32, (block, block), 1)
    lower = r_id >= c_id
    upper = r_id <= c_id
    cum_f = dot(keep, upper.astype(F32), precision=HIGHEST)[1:2]
    cum_b = dot(keep, lower.astype(F32), precision=HIGHEST)[3:4]
    a_f = gates[0:1] - cum_f
    a_b = gates[2:3] - cum_b
    end_f = cum_f[:, block - 1 : block]
    end_b = cum_b[:, 0:1]
    peak_f = jnp.max(end_f + a_f, axis=1, keepdims=True)
    peak_b = jnp.max(end_b + a_b, axis=1, keepdims=True)
    e_f = jnp.exp(end_f + a_f - peak_f)
    e_b = jnp.exp(end_b + a_b - peak_b)
    row8 = lax.broadcasted_iota(jnp.int32, (8, block), 0)
    stack = jnp.where(
        row8 == 0,
        cum_f,
        jnp.where(row8 == 1, cum_b, jnp.where(row8 == 2, e_f, e_b)),
    )
    eye = (r_id == c_id).astype(F32)
    columns = dot_t(eye, stack, precision=HIGHEST)
    cum_f_col = columns[:, 0:1]
    cum_b_col = columns[:, 1:2]
    e_f_col = columns[:, 2:3]
    e_b_col = columns[:, 3:4]

    k = dot_t(x, get("key_rows")[...]).astype(BF16).astype(F32)
    k = k * k.shape[1] ** (-0.5)
    v = dot(x, get("rec_value")[...]).astype(BF16)
    k16 = k.astype(BF16)
    mk = k.shape[1]
    mv = v.shape[1]
    n_both = dot(stack.astype(BF16), k16)
    row16 = lax.broadcasted_iota(jnp.int32, (16, mv), 0)

    def put_state(d, e_col, n_row, peak, end):
        smsg[d, :mk, :] = dot_tn((k * e_col).astype(BF16), v).astype(BF16)
        p1, p2, p3 = three_terms(peak)
        f1, f2, f3 = three_terms(end)
        tail = jnp.concatenate([n_row, jnp.zeros((1, mv - mk), F32)], axis=1)
        tail = jnp.where(row16 == 0, tail, 0.0)
        for at, term in enumerate((p1, p2, p3, f1, f2, f3)):
            tail = jnp.where(row16 == at + 1, term, tail)
        smsg[d, mk:, :] = tail.astype(BF16)

    put_state(0, e_f_col, n_both[2:3], peak_f, end_f)
    put_state(1, e_b_col, n_both[3:4], peak_b, end_b)

    def s_copy(i):
        to = lax.rem(sp + i, n_sp)
        which = jnp.where(to > sp, 0, 1)
        return remote(smsg.at[which], sbuf.at[sp], s_send.at[i], s_recv.at[sp], (to, tp))

    def start_s(i, c):
        s_copy(i).start()
        return c

    lax.fori_loop(1, n_sp, start_s, 0)

    q_latent = rms(dot(x, get("query_down")[...]), get("query_gain")[...]).astype(BF16)
    q_nope = dot(q_latent, get("query_nope_up")[...]).astype(BF16)
    q_rope = dot_t(q_latent, get("query_rope_rows")[...])
    cos_q = cos_b * cos_l[...] - sin_b * sin_l[...]
    sin_q = sin_b * cos_l[...] + cos_b * sin_l[...]
    q_rope = q_rope * cos_q + turned(q_rope) * sin_q
    qcat[:, :lat] = dot_t(q_nope, get("key_up")[...]).astype(BF16)
    qcat[:, lat:] = jnp.concatenate([q_rope, jnp.zeros_like(q_rope)], axis=1).astype(BF16)
    scale = (q_nope.shape[1] + rope) ** (-0.5)

    def relay(i, c):
        slot = slot_of(i)
        remote(
            kvbuf.at[slot], kvbuf.at[slot], kv_send.at[i], kv_recv.at[slot], partner
        ).wait_recv()
        kv_relay(i).start()
        return c

    lax.fori_loop(1, plane, relay, 0)

    q16 = dot_t(x, get("query_rows")[...]).astype(BF16)
    qf = q16.astype(F32)
    qk = dot_t(q16, k16)

    def within(mask, cum_col, a_row):
        decay = jnp.where(mask, cum_col + a_row, NEG)
        top = jnp.max(decay, axis=1, keepdims=True)
        gated = qk * jnp.exp(decay - top)
        return top, dot(gated.astype(BF16), v), jnp.sum(gated, axis=1, keepdims=True)

    in_f = within(lower, cum_f_col, a_f)
    in_b = within(upper, cum_b_col, a_b)

    def wait_kv(i, c):
        s = i // half
        t = 2 * lax.rem(i, half) + 1 - parity
        slot = s * n_tp + t
        remote(
            kvbuf.at[slot], kvbuf.at[slot], kv_fwd.at[0], kv_recv.at[slot], partner
        ).wait_recv()
        return c

    lax.fori_loop(0, plane, wait_kv, 0)
    queries = qcat[...]
    slots = n_sp * n_tp
    step = min(slots, 32)

    def attend(j, running):
        peak, mass, accum = running
        keys = kvbuf[pl.ds(j * step, step)].reshape(step * rows, kvbuf.shape[2])
        scores = dot_t(queries, keys) * scale
        new = jnp.maximum(peak, jnp.max(scores, axis=1, keepdims=True))
        expo = jnp.exp(scores - new)
        shrink = jnp.exp(peak - new)
        mass = mass * shrink + jnp.sum(expo, axis=1, keepdims=True)
        accum = accum * shrink + dot(expo.astype(BF16), keys[:, :lat])
        return new, mass, accum

    running = (
        jnp.full((block, 1), NEG, F32),
        jnp.zeros((block, 1), F32),
        jnp.zeros((block, lat), F32),
    )
    if slots == step:
        running = attend(0, running)
    else:
        running = lax.fori_loop(0, slots // step, attend, running)
    attended = (running[2] / running[1]).astype(BF16)
    vh = hbm["value_up"].shape[1]
    mix[:, :vh] = dot(attended, get("value_up")[...]).astype(BF16)

    w_attn = get("out_attn")
    w_rec = get("out_rec")
    pfull[...] = dot(mix[:, :vh], w_attn[...]).reshape(pfull.shape)

    def absorb(j, state):
        c_state, n_state, m_state = state
        remote(smsg.at[0], sbuf.at[j], s_send.at[0], s_recv.at[j], partner).wait_recv()
        c_new = sbuf[j, :mk, :].astype(F32)
        tail = sbuf[j, mk:, :].astype(F32)
        peak = tail[1:2, 0:1] + tail[2:3, 0:1] + tail[3:4, 0:1]
        end = tail[4:5, 0:1] + tail[5:6, 0:1] + tail[6:7, 0:1]
        top = jnp.maximum(end + m_state, peak)
        carried = jnp.exp(end + m_state - top)
        fresh = jnp.exp(peak - top)
        return (
            carried * c_state + fresh * c_new,
            carried * n_state + fresh * tail[0:1, :mk],
            top,
        )

    state0 = get("init_state")
    norm0 = get("init_norm")
    zero = jnp.zeros((1, 1), F32)
    fwd = lax.fori_loop(0, sp, absorb, (state0[0], norm0[0:1], zero))
    bwd = lax.fori_loop(
        0,
        n_sp - 1 - sp,
        lambda j, state: absorb(n_sp - 1 - j, state),
        (state0[1], norm0[1:2], zero),
    )
    floor = float(n_sp * block) ** 0.5

    def finish(inside, cum_col, state):
        top, num, den = inside
        c_state, n_state, m_state = state
        carry = cum_col + m_state
        new = jnp.maximum(top, carry)
        a = jnp.exp(top - new)
        b = jnp.exp(carry - new)
        num = a * num + b * dot(q16, c_state.astype(BF16))
        den = a * den + b * jnp.sum(qf * n_state, axis=1, keepdims=True)
        return num / jnp.maximum(jnp.abs(den), floor * jnp.exp(-new))

    total = finish(in_f, cum_f_col, fwd) + finish(in_b, cum_b_col, bwd)
    mix[:, vh:] = rms(total, get("head_gain")[...]).astype(BF16)

    width = pfull.shape[2]
    strip = width // STRIPS
    p_out = []
    l_out = []
    for c in range(STRIPS):
        cols = slice(c * strip, (c + 1) * strip)
        add = dot(mix[:, vh:], w_rec[:, cols]).reshape(n_tp, rows, strip)
        pfull[:, :, cols] = pfull[:, :, cols] + add
        for d in range(half):
            to = lax.rem(partner_t + 2 * (d + 1), n_tp)
            psend[d, c] = pfull[to, :, cols].astype(BF16)
            at = c * half + d
            copy = remote(psend.at[d, c], prem.at[d, c], p_send.at[at], p_recv.at[at], partner)
            copy.start()
            p_out.append(copy)
    for c in range(STRIPS):
        cols = slice(c * strip, (c + 1) * strip)
        for d in range(half - 1):
            at = c * half + d
            p_out[at].wait_recv()
            to = tp_same(d + 1)
            plast[d, c] = (pfull[to, :, cols] + prem[d, c].astype(F32)).astype(BF16)
            copy = remote(
                plast.at[d, c], plast_in.at[d, c], l_send.at[at], l_recv.at[at], (sp, to)
            )
            copy.start()
            l_out.append(copy)
    for c in range(STRIPS):
        cols = slice(c * strip, (c + 1) * strip)
        p_out[c * half + half - 1].wait_recv()
        both = pfull[tp, :, cols] + prem[half - 1, c].astype(F32)
        for d in range(half - 1):
            l_out[c * (half - 1) + d].wait_recv()
            both = both + plast_in[d, c].astype(F32)
        out_ref[:, cols] = both.astype(BF16)

    for copy in x_out + x_fwd + p_out + l_out:
        copy.wait_send()

    def drain_kv(i, c):
        kv_copy(i).wait_send()
        return c

    def drain_relay(i, c):
        kv_relay(i).wait_send()
        return c

    def drain_s(i, c):
        s_copy(i).wait_send()
        return c

    lax.fori_loop(1, plane, drain_kv, 0)
    lax.fori_loop(0, plane, drain_relay, 0)
    lax.fori_loop(1, n_sp, drain_s, 0)


ORDER = (
    "rows_in",
    "in_gain",
    "kv_down",
    "kv_gain",
    "rope_rows",
    "cos_local",
    "sin_local",
    "cos_base",
    "sin_base",
    "gate_rows",
    "levels",
    "key_rows",
    "rec_value",
    "query_down",
    "query_gain",
    "query_nope_up",
    "query_rope_rows",
    "key_up",
    "query_rows",
    "value_up",
    "init_state",
    "init_norm",
    "head_gain",
    "out_attn",
    "out_rec",
)


def shards(
    n_sp,
    n_tp,
    rows_in,
    in_gain,
    query_down,
    query_gain,
    kv_down,
    kv_gain,
    rope_down,
    query_nope_up,
    query_rope_up,
    key_up,
    value_up,
    rec_query,
    rec_key,
    rec_value,
    gate_weight,
    forget_level,
    head_gain,
    init_state,
    init_norm,
    out_attn,
    out_rec,
):
    rows, width = rows_in.shape
    block = forget_level.shape[0]
    lat = kv_down.shape[1]
    rope = rope_down.shape[1]
    mk = rec_key.shape[1]
    mv = rec_value.shape[1]
    half = n_tp // 2
    pair = rope // 2
    frequency = 10000.0 ** (-np.arange(pair) / pair)
    frequency = np.concatenate([frequency, frequency])
    local = np.arange(block)[:, None] * frequency
    base = (np.arange(n_sp) * block)[:, None, None] * frequency
    arrays = dict(
        rows_in=rows_in,
        in_gain=in_gain[None],
        kv_down=kv_down,
        kv_gain=kv_gain[None],
        rope_rows=rope_down.T,
        cos_local=jnp.asarray(np.cos(local), F32),
        sin_local=jnp.asarray(np.sin(local), F32),
        cos_base=jnp.asarray(np.cos(base), F32),
        sin_base=jnp.asarray(np.sin(base), F32),
        gate_rows=gate_weight[:, :, 0].T,
        levels=forget_level.transpose(1, 2, 0),
        key_rows=rec_key.T,
        rec_value=rec_value,
        query_down=query_down,
        query_gain=query_gain[None],
        query_nope_up=query_nope_up,
        query_rope_rows=query_rope_up.T,
        key_up=key_up,
        query_rows=rec_query.T,
        value_up=value_up,
        init_state=init_state[:, 0],
        init_norm=init_norm[:, 0],
        head_gain=head_gain[None],
        out_attn=out_attn,
        out_rec=out_rec,
    )
    operands = [arrays[name] for name in ORDER]
    plane = n_sp * half
    slots = n_sp * n_tp
    dma = pltpu.SemaphoreType.DMA
    scratch = [pltpu.VMEM(a.shape, a.dtype) for a in operands]
    scratch += [
        pltpu.VMEM((n_tp, rows, width), BF16),
        pltpu.VMEM((slots, rows, lat + 2 * rope), BF16),
        pltpu.VMEM((block, lat + 2 * rope), BF16),
        pltpu.VMEM((block, value_up.shape[1] + mv), BF16),
        pltpu.VMEM((2, mk + 16, mv), BF16),
        pltpu.VMEM((n_sp, mk + 16, mv), BF16),
        pltpu.VMEM((half, STRIPS, rows, width // STRIPS), BF16),
        pltpu.VMEM((n_tp, rows, width), F32),
        pltpu.VMEM((half, STRIPS, rows, width // STRIPS), BF16),
        pltpu.VMEM((half, STRIPS, rows, width // STRIPS), BF16),
        pltpu.VMEM((half, STRIPS, rows, width // STRIPS), BF16),
        dma((len(operands),)),
        dma((n_tp,)),
        dma((n_tp,)),
        dma((plane,)),
        dma((plane,)),
        dma((slots,)),
        dma((n_sp,)),
        dma((n_sp,)),
        dma((half * STRIPS,)),
        dma((half * STRIPS,)),
        dma((half * STRIPS,)),
        dma((half * STRIPS,)),
    ]
    return pl.pallas_call(
        functools.partial(kernel, n_sp, n_tp, ORDER),
        out_shape=jax.ShapeDtypeStruct((rows, width), BF16),
        in_specs=[pl.BlockSpec(memory_space=pl.ANY)] * len(operands),
        out_specs=pl.BlockSpec(memory_space=pltpu.VMEM),
        scratch_shapes=scratch,
        compiler_params=pltpu.CompilerParams(
            collective_id=0, has_side_effects=True, vmem_limit_bytes=60 * 2**20
        ),
    )(*operands)


def solution(mesh):
    in_specs = (
        P(("sp", "tp"), None),
        P(),
        P(),
        P(),
        P(),
        P(),
        P(),
        P(None, "tp"),
        P(None, "tp"),
        P(None, "tp"),
        P(None, "tp"),
        P(None, "tp"),
        P(None, "tp"),
        P(None, "tp"),
        P(None, None, "tp"),
        P("sp", None, "tp"),
        P("tp"),
        P(None, "tp", None, None),
        P(None, "tp", None),
        P("tp", None),
        P("tp", None),
    )
    return jax.shard_map(
        functools.partial(shards, mesh.shape["sp"], mesh.shape["tp"]),
        mesh=mesh,
        in_specs=in_specs,
        out_specs=P(("sp", "tp"), None),
        check_vma=False,
    )
```

```python
import functools

import jax
import jax.numpy as jnp
import numpy as np
from jax import lax
from jax.experimental import pallas as pl
from jax.experimental.pallas import tpu as pltpu
from jax.sharding import PartitionSpec as P

EPS = 1e-06
NEG = -1e30
HIGHEST = lax.Precision.HIGHEST
MESH = pl.DeviceIdType.MESH
F32 = jnp.float32
BF16 = jnp.bfloat16
STRIPS = 4


def dot(a, b, **kw):
    return jnp.dot(a, b, preferred_element_type=F32, **kw)


def dot_t(a, b, **kw):
    return lax.dot_general(a, b, (((1,), (1,)), ((), ())), preferred_element_type=F32, **kw)


def dot_tn(a, b, **kw):
    return lax.dot_general(a, b, (((0,), (0,)), ((), ())), preferred_element_type=F32, **kw)


def rms(values, gains):
    return values * lax.rsqrt(jnp.mean(values * values, axis=-1, keepdims=True) + EPS) * gains


def turned(values):
    half = values.shape[-1] // 2
    return jnp.concatenate([-values[:, half:], values[:, :half]], axis=1)


def three_terms(value):
    high = value.astype(BF16).astype(F32)
    mid = (value - high).astype(BF16).astype(F32)
    return high, mid, value - high - mid


def kernel(n_sp, n_tp, names, *refs):
    count = len(names)
    hbm = dict(zip(names, refs[:count]))
    out_ref = refs[count]
    vm = dict(zip(names, refs[count + 1 : 2 * count + 1]))
    (
        xall,
        kvbuf,
        qcat,
        mix,
        smsg,
        sbuf,
        psend,
        pfull,
        prem,
        plast,
        plast_in,
        load_sem,
        x_send,
        x_recv,
        kv_send,
        kv_fwd,
        kv_recv,
        s_send,
        s_recv,
        p_send,
        p_recv,
        l_send,
        l_recv,
    ) = refs[2 * count + 1 :]
    half = n_tp // 2
    sp = lax.axis_index("sp")
    tp = lax.axis_index("tp")
    parity = lax.rem(tp, 2)
    partner_t = tp + 1 - 2 * parity
    partner = (sp, partner_t)
    rows = xall.shape[1]
    block = n_tp * rows
    plane = n_sp * half
    mine = sp * half + tp // 2

    loads = {
        name: pltpu.make_async_copy(hbm[name], vm[name], load_sem.at[i])
        for i, name in enumerate(names)
    }
    for name in names:
        loads[name].start()

    def peer_of(i):
        linear = lax.rem(mine + i, plane)
        return (linear // half, 2 * lax.rem(linear, half) + parity)

    barrier = pltpu.get_barrier_semaphore()

    def greet(i, c):
        pl.semaphore_signal(barrier, inc=1, device_id=peer_of(i), device_id_type=MESH)
        return c

    lax.fori_loop(1, plane, greet, 0)
    pl.semaphore_signal(barrier, inc=1, device_id=partner, device_id_type=MESH)

    def get(name):
        loads[name].wait()
        return vm[name]

    rows_in = get("rows_in")
    in_gain = get("in_gain")
    xall[tp] = rms(rows_in[...].astype(F32), in_gain[...]).astype(BF16)
    pl.semaphore_wait(barrier, plane)

    def remote(src, dst, send, recv, device):
        return pltpu.make_async_remote_copy(
            src_ref=src,
            dst_ref=dst,
            send_sem=send,
            recv_sem=recv,
            device_id=device,
            device_id_type=MESH,
        )

    def x_copy(slot, k, device):
        return remote(xall.at[slot], xall.at[slot], x_send.at[k], x_recv.at[slot], device)

    def tp_same(d):
        return lax.rem(tp + 2 * d, n_tp)

    x_out = []
    for d in range(1, half):
        x_out.append(x_copy(tp, d, (sp, tp_same(d))))
    x_out.append(x_copy(tp, 0, partner))
    for copy in x_out:
        copy.start()

    own = xall[tp]
    cos_l = get("cos_local")
    sin_l = get("sin_local")
    cos_b = get("cos_base")[sp]
    sin_b = get("sin_base")[sp]
    own_at = pl.ds(pl.multiple_of(tp * rows, rows), rows)
    kv = rms(dot(own, get("kv_down")[...]), get("kv_gain")[...])
    kr = dot_t(own, get("rope_rows")[...])
    c_l = cos_l[own_at, :]
    s_l = sin_l[own_at, :]
    kr = kr * (cos_b * c_l - sin_b * s_l) + turned(kr) * (sin_b * c_l + cos_b * s_l)
    lat = kv.shape[1]
    rope = kr.shape[1]
    slot_me = sp * n_tp + tp
    kvbuf[slot_me, :, :lat] = kv.astype(BF16)
    kvbuf[slot_me, :, lat:] = jnp.concatenate([kr, jnp.zeros_like(kr)], axis=1).astype(BF16)

    def kv_copy(i):
        return remote(
            kvbuf.at[slot_me], kvbuf.at[slot_me], kv_send.at[i], kv_recv.at[slot_me], peer_of(i)
        )

    def slot_of(i):
        s, t = peer_of(i)
        return s * n_tp + t

    def kv_relay(i):
        slot = slot_of(i)
        return remote(kvbuf.at[slot], kvbuf.at[slot], kv_fwd.at[i], kv_recv.at[slot], partner)

    def start_kv(i, c):
        kv_copy(i).start()
        return c

    lax.fori_loop(1, plane, start_kv, 0)
    kv_relay(0).start()

    x_fwd = []
    for d in range(1, half):
        slot = tp_same(d)
        x_copy(slot, 0, partner).wait_recv()
        copy = x_copy(slot, half + d, partner)
        copy.start()
        x_fwd.append(copy)
    for d in range(half):
        x_copy(lax.rem(partner_t + 2 * d, n_tp), 0, partner).wait_recv()
    x = xall[...].reshape(block, xall.shape[2])

    gates = dot_t(get("gate_rows")[...], x)
    levels = get("levels")
    row4 = lax.broadcasted_iota(jnp.int32, gates.shape, 0)
    level = gates + jnp.where(row4 < 2, levels[0], levels[1])
    keep = jnp.minimum(level, 0.0) - jnp.log1p(jnp.exp(-jnp.abs(level)))
    r_id = lax.broadcasted_iota(jnp.int32, (block, block), 0)
    c_id = lax.broadcasted_iota(jnp.int32, (block, block), 1)
    lower = r_id >= c_id
    upper = r_id <= c_id
    cum_f = dot(keep, upper.astype(F32), precision=HIGHEST)[1:2]
    cum_b = dot(keep, lower.astype(F32), precision=HIGHEST)[3:4]
    a_f = gates[0:1] - cum_f
    a_b = gates[2:3] - cum_b
    end_f = cum_f[:, block - 1 : block]
    end_b = cum_b[:, 0:1]
    peak_f = jnp.max(end_f + a_f, axis=1, keepdims=True)
    peak_b = jnp.max(end_b + a_b, axis=1, keepdims=True)
    e_f = jnp.exp(end_f + a_f - peak_f)
    e_b = jnp.exp(end_b + a_b - peak_b)
    row8 = lax.broadcasted_iota(jnp.int32, (8, block), 0)
    stack = jnp.where(
        row8 == 0,
        cum_f,
        jnp.where(row8 == 1, cum_b, jnp.where(row8 == 2, e_f, e_b)),
    )
    eye = (r_id == c_id).astype(F32)
    columns = dot_t(eye, stack, precision=HIGHEST)
    cum_f_col = columns[:, 0:1]
    cum_b_col = columns[:, 1:2]
    e_f_col = columns[:, 2:3]
    e_b_col = columns[:, 3:4]

    k = dot_t(x, get("key_rows")[...]).astype(BF16).astype(F32)
    k = k * k.shape[1] ** (-0.5)
    v = dot(x, get("rec_value")[...]).astype(BF16)
    k16 = k.astype(BF16)
    mk = k.shape[1]
    mv = v.shape[1]
    n_both = dot(stack.astype(BF16), k16)
    row16 = lax.broadcasted_iota(jnp.int32, (16, mv), 0)

    def put_state(d, e_col, n_row, peak, end):
        smsg[d, :mk, :] = dot_tn((k * e_col).astype(BF16), v).astype(BF16)
        p1, p2, p3 = three_terms(peak)
        f1, f2, f3 = three_terms(end)
        tail = jnp.concatenate([n_row, jnp.zeros((1, mv - mk), F32)], axis=1)
        tail = jnp.where(row16 == 0, tail, 0.0)
        for at, term in enumerate((p1, p2, p3, f1, f2, f3)):
            tail = jnp.where(row16 == at + 1, term, tail)
        smsg[d, mk:, :] = tail.astype(BF16)

    put_state(0, e_f_col, n_both[2:3], peak_f, end_f)
    put_state(1, e_b_col, n_both[3:4], peak_b, end_b)

    def s_copy(i):
        to = lax.rem(sp + i, n_sp)
        which = jnp.where(to > sp, 0, 1)
        return remote(smsg.at[which], sbuf.at[sp], s_send.at[i], s_recv.at[sp], (to, tp))

    def start_s(i, c):
        s_copy(jnp.where(2 * sp < n_sp, n_sp - i, i)).start()
        return c

    lax.fori_loop(1, n_sp, start_s, 0)

    q_latent = rms(dot(x, get("query_down")[...]), get("query_gain")[...]).astype(BF16)
    q_nope = dot(q_latent, get("query_nope_up")[...]).astype(BF16)
    q_rope = dot_t(q_latent, get("query_rope_rows")[...])
    cos_q = cos_b * cos_l[...] - sin_b * sin_l[...]
    sin_q = sin_b * cos_l[...] + cos_b * sin_l[...]
    q_rope = q_rope * cos_q + turned(q_rope) * sin_q
    qcat[:, :lat] = dot_t(q_nope, get("key_up")[...]).astype(BF16)
    qcat[:, lat:] = jnp.concatenate([q_rope, jnp.zeros_like(q_rope)], axis=1).astype(BF16)
    scale = (q_nope.shape[1] + rope) ** (-0.5)

    def relay(i, c):
        slot = slot_of(i)
        remote(
            kvbuf.at[slot], kvbuf.at[slot], kv_send.at[i], kv_recv.at[slot], partner
        ).wait_recv()
        kv_relay(i).start()
        return c

    lax.fori_loop(1, plane, relay, 0)

    q16 = dot_t(x, get("query_rows")[...]).astype(BF16)
    qf = q16.astype(F32)
    qk = dot_t(q16, k16)

    def within(mask, cum_col, a_row):
        decay = jnp.where(mask, cum_col + a_row, NEG)
        top = jnp.max(decay, axis=1, keepdims=True)
        gated = qk * jnp.exp(decay - top)
        return top, dot(gated.astype(BF16), v), jnp.sum(gated, axis=1, keepdims=True)

    in_f = within(lower, cum_f_col, a_f)
    in_b = within(upper, cum_b_col, a_b)

    def wait_kv(i, c):
        s = i // half
        t = 2 * lax.rem(i, half) + 1 - parity
        slot = s * n_tp + t
        remote(
            kvbuf.at[slot], kvbuf.at[slot], kv_fwd.at[0], kv_recv.at[slot], partner
        ).wait_recv()
        return c

    lax.fori_loop(0, plane, wait_kv, 0)
    queries = qcat[...]
    slots = n_sp * n_tp
    step = min(slots, 32)

    def attend(j, running):
        peak, mass, accum = running
        keys = kvbuf[pl.ds(j * step, step)].reshape(step * rows, kvbuf.shape[2])
        scores = dot_t(queries, keys) * scale
        new = jnp.maximum(peak, jnp.max(scores, axis=1, keepdims=True))
        expo = jnp.exp(scores - new)
        shrink = jnp.exp(peak - new)
        mass = mass * shrink + jnp.sum(expo, axis=1, keepdims=True)
        accum = accum * shrink + dot(expo.astype(BF16), keys[:, :lat])
        return new, mass, accum

    running = (
        jnp.full((block, 1), NEG, F32),
        jnp.zeros((block, 1), F32),
        jnp.zeros((block, lat), F32),
    )
    if slots == step:
        running = attend(0, running)
    else:
        running = lax.fori_loop(0, slots // step, attend, running)
    attended = (running[2] / running[1]).astype(BF16)
    vh = hbm["value_up"].shape[1]
    mix[:, :vh] = dot(attended, get("value_up")[...]).astype(BF16)

    w_attn = get("out_attn")
    w_rec = get("out_rec")
    pfull[...] = dot(mix[:, :vh], w_attn[...]).reshape(pfull.shape)

    def absorb(j, state):
        c_state, n_state, m_state, f_state = state
        remote(smsg.at[0], sbuf.at[j], s_send.at[0], s_recv.at[j], partner).wait_recv()
        c_new = sbuf[j, :mk, :].astype(F32)
        tail = sbuf[j, mk:, :].astype(F32)
        peak = tail[1:2, 0:1] + tail[2:3, 0:1] + tail[3:4, 0:1] + f_state
        end = tail[4:5, 0:1] + tail[5:6, 0:1] + tail[6:7, 0:1]
        top = jnp.maximum(m_state, peak)
        kept = jnp.exp(m_state - top)
        fresh = jnp.exp(peak - top)
        return (
            kept * c_state + fresh * c_new,
            kept * n_state + fresh * tail[0:1, :mk],
            top,
            f_state + end,
        )

    def with_start(state, c_start, n_start):
        c_state, n_state, m_state, f_state = state
        top = jnp.maximum(m_state, f_state)
        kept = jnp.exp(m_state - top)
        carried = jnp.exp(f_state - top)
        return (
            kept * c_state + carried * c_start,
            kept * n_state + carried * n_start,
            top,
        )

    state0 = get("init_state")
    norm0 = get("init_norm")
    empty = (
        jnp.zeros((mk, mv), F32),
        jnp.zeros((1, mk), F32),
        jnp.full((1, 1), NEG, F32),
        jnp.zeros((1, 1), F32),
    )
    fwd = lax.fori_loop(0, sp, lambda i, state: absorb(sp - 1 - i, state), empty)
    bwd = lax.fori_loop(sp + 1, n_sp, absorb, empty)
    fwd = with_start(fwd, state0[0], norm0[0:1])
    bwd = with_start(bwd, state0[1], norm0[1:2])
    floor = float(n_sp * block) ** 0.5

    def finish(inside, cum_col, state):
        top, num, den = inside
        c_state, n_state, m_state = state
        carry = cum_col + m_state
        new = jnp.maximum(top, carry)
        a = jnp.exp(top - new)
        b = jnp.exp(carry - new)
        num = a * num + b * dot(q16, c_state.astype(BF16))
        den = a * den + b * jnp.sum(qf * n_state, axis=1, keepdims=True)
        return num / jnp.maximum(jnp.abs(den), floor * jnp.exp(-new))

    total = finish(in_f, cum_f_col, fwd) + finish(in_b, cum_b_col, bwd)
    mix[:, vh:] = rms(total, get("head_gain")[...]).astype(BF16)

    width = pfull.shape[2]
    strip = width // STRIPS
    p_out = []
    l_out = []
    for c in range(STRIPS):
        cols = slice(c * strip, (c + 1) * strip)
        add = dot(mix[:, vh:], w_rec[:, cols]).reshape(n_tp, rows, strip)
        pfull[:, :, cols] = pfull[:, :, cols] + add
        for d in range(half):
            to = lax.rem(partner_t + 2 * (d + 1), n_tp)
            psend[d, c] = pfull[to, :, cols].astype(BF16)
            at = c * half + d
            copy = remote(psend.at[d, c], prem.at[d, c], p_send.at[at], p_recv.at[at], partner)
            copy.start()
            p_out.append(copy)
    for c in range(STRIPS):
        cols = slice(c * strip, (c + 1) * strip)
        for d in range(half - 1):
            at = c * half + d
            p_out[at].wait_recv()
            to = tp_same(d + 1)
            plast[d, c] = (pfull[to, :, cols] + prem[d, c].astype(F32)).astype(BF16)
            copy = remote(
                plast.at[d, c], plast_in.at[d, c], l_send.at[at], l_recv.at[at], (sp, to)
            )
            copy.start()
            l_out.append(copy)
    for c in range(STRIPS):
        cols = slice(c * strip, (c + 1) * strip)
        p_out[c * half + half - 1].wait_recv()
        both = pfull[tp, :, cols] + prem[half - 1, c].astype(F32)
        for d in range(half - 1):
            l_out[c * (half - 1) + d].wait_recv()
            both = both + plast_in[d, c].astype(F32)
        out_ref[:, cols] = both

    for copy in x_out + x_fwd + p_out + l_out:
        copy.wait_send()

    def drain_kv(i, c):
        kv_copy(i).wait_send()
        return c

    def drain_relay(i, c):
        kv_relay(i).wait_send()
        return c

    def drain_s(i, c):
        s_copy(i).wait_send()
        return c

    lax.fori_loop(1, plane, drain_kv, 0)
    lax.fori_loop(0, plane, drain_relay, 0)
    lax.fori_loop(1, n_sp, drain_s, 0)


ORDER = (
    "rows_in",
    "in_gain",
    "kv_down",
    "kv_gain",
    "rope_rows",
    "cos_local",
    "sin_local",
    "cos_base",
    "sin_base",
    "gate_rows",
    "levels",
    "key_rows",
    "rec_value",
    "query_down",
    "query_gain",
    "query_nope_up",
    "query_rope_rows",
    "key_up",
    "query_rows",
    "value_up",
    "init_state",
    "init_norm",
    "head_gain",
    "out_attn",
    "out_rec",
)


def shards(
    n_sp,
    n_tp,
    rows_in,
    in_gain,
    query_down,
    query_gain,
    kv_down,
    kv_gain,
    rope_down,
    query_nope_up,
    query_rope_up,
    key_up,
    value_up,
    rec_query,
    rec_key,
    rec_value,
    gate_weight,
    forget_level,
    head_gain,
    init_state,
    init_norm,
    out_attn,
    out_rec,
):
    rows, width = rows_in.shape
    block = forget_level.shape[0]
    lat = kv_down.shape[1]
    rope = rope_down.shape[1]
    mk = rec_key.shape[1]
    mv = rec_value.shape[1]
    half = n_tp // 2
    pair = rope // 2
    frequency = 10000.0 ** (-np.arange(pair) / pair)
    frequency = np.concatenate([frequency, frequency])
    local = np.arange(block)[:, None] * frequency
    base = (np.arange(n_sp) * block)[:, None, None] * frequency
    arrays = dict(
        rows_in=rows_in,
        in_gain=in_gain[None],
        kv_down=kv_down,
        kv_gain=kv_gain[None],
        rope_rows=rope_down.T,
        cos_local=jnp.asarray(np.cos(local), F32),
        sin_local=jnp.asarray(np.sin(local), F32),
        cos_base=jnp.asarray(np.cos(base), F32),
        sin_base=jnp.asarray(np.sin(base), F32),
        gate_rows=gate_weight[:, :, 0].T,
        levels=forget_level.transpose(1, 2, 0),
        key_rows=rec_key.T,
        rec_value=rec_value,
        query_down=query_down,
        query_gain=query_gain[None],
        query_nope_up=query_nope_up,
        query_rope_rows=query_rope_up.T,
        key_up=key_up,
        query_rows=rec_query.T,
        value_up=value_up,
        init_state=init_state[:, 0],
        init_norm=init_norm[:, 0],
        head_gain=head_gain[None],
        out_attn=out_attn,
        out_rec=out_rec,
    )
    operands = [arrays[name] for name in ORDER]
    plane = n_sp * half
    slots = n_sp * n_tp
    dma = pltpu.SemaphoreType.DMA
    scratch = [pltpu.VMEM(a.shape, a.dtype) for a in operands]
    scratch += [
        pltpu.VMEM((n_tp, rows, width), BF16),
        pltpu.VMEM((slots, rows, lat + 2 * rope), BF16),
        pltpu.VMEM((block, lat + 2 * rope), BF16),
        pltpu.VMEM((block, value_up.shape[1] + mv), BF16),
        pltpu.VMEM((2, mk + 16, mv), BF16),
        pltpu.VMEM((n_sp, mk + 16, mv), BF16),
        pltpu.VMEM((half, STRIPS, rows, width // STRIPS), BF16),
        pltpu.VMEM((n_tp, rows, width), F32),
        pltpu.VMEM((half, STRIPS, rows, width // STRIPS), BF16),
        pltpu.VMEM((half, STRIPS, rows, width // STRIPS), BF16),
        pltpu.VMEM((half, STRIPS, rows, width // STRIPS), BF16),
        dma((len(operands),)),
        dma((n_tp,)),
        dma((n_tp,)),
        dma((plane,)),
        dma((plane,)),
        dma((slots,)),
        dma((n_sp,)),
        dma((n_sp,)),
        dma((half * STRIPS,)),
        dma((half * STRIPS,)),
        dma((half * STRIPS,)),
        dma((half * STRIPS,)),
    ]
    total = pl.pallas_call(
        functools.partial(kernel, n_sp, n_tp, ORDER),
        out_shape=jax.ShapeDtypeStruct((rows, width), F32),
        in_specs=[pl.BlockSpec(memory_space=pl.ANY)] * len(operands),
        out_specs=pl.BlockSpec(memory_space=pltpu.VMEM),
        scratch_shapes=scratch,
        compiler_params=pltpu.CompilerParams(
            collective_id=0, has_side_effects=True, vmem_limit_bytes=60 * 2**20
        ),
    )(*operands)
    return total.astype(BF16)


def solution(mesh):
    in_specs = (
        P(("sp", "tp"), None),
        P(),
        P(),
        P(),
        P(),
        P(),
        P(),
        P(None, "tp"),
        P(None, "tp"),
        P(None, "tp"),
        P(None, "tp"),
        P(None, "tp"),
        P(None, "tp"),
        P(None, "tp"),
        P(None, None, "tp"),
        P("sp", None, "tp"),
        P("tp"),
        P(None, "tp", None, None),
        P(None, "tp", None),
        P("tp", None),
        P("tp", None),
    )
    return jax.shard_map(
        functools.partial(shards, mesh.shape["sp"], mesh.shape["tp"]),
        mesh=mesh,
        in_specs=in_specs,
        out_specs=P(("sp", "tp"), None),
        check_vma=False,
    )
```
